128 devices in a mesh: ep: 128 (over z, y, x, core).
Axes of the slice: x: 4, y: 4, z: 4, core: 2. Of those that a mesh axis runs over, the one named last changes fastest.
Arguments:
- tokens: bfloat16 [1024, 2048], P('ep'), may hold values from -6 to 6
- cache_keys: bfloat16 [1024, 1024, 128], P('ep'), may hold values from -80 to 80
- cache_values: bfloat16 [1024, 1024, 128], P('ep'), may hold values from -6 to 6
- cum_gates: float32 [1024, 1024, 2], P('ep'), may hold values from -1024 to 0, as said below
- lengths: int32 [1024], P('ep'), may hold values from 128 to 1024
- query_weight: bfloat16 [2048, 2048], replicated, may hold values from -0.125 to 0.125
- key_weight: bfloat16 [2048, 128], replicated, may hold values from -0.125 to 0.125
- value_weight: bfloat16 [2048, 128], replicated, may hold values from -0.125 to 0.125
- forget_weight: bfloat16 [2048, 2], replicated, may hold values from -0.125 to 0.125
- out_weight: bfloat16 [2048, 2048], P('ep'), may hold values from -1 to 1
- norm_gain: float32 [2, 2048], replicated, may hold values from 0.1 to 1.9
- norm_bias: float32 [2, 2048], replicated, may hold values from -1 to 1
- dense_gate_weight: bfloat16 [2048, 5632], P(None, 'ep'), may hold values from -0.125 to 0.125
- dense_up_weight: bfloat16 [2048, 5632], P(None, 'ep'), may hold values from -0.125 to 0.125
- dense_down_weight: bfloat16 [5632, 2048], P('ep'), may hold values from -0.078125 to 0.078125
- dense_scale: float32 [2048], replicated, may hold values from 0.2 to 1.5
- expert_gate_weight: bfloat16 [2048, 57344], P(None, 'ep'), may hold values from -0.125 to 0.125
- expert_up_weight: bfloat16 [2048, 57344], P(None, 'ep'), may hold values from -0.125 to 0.125
- expert_down_weight: bfloat16 [57344, 2048], P('ep'), may hold values from -0.0625 to 0.0625
- routes: int32 [1024, 2], replicated, may hold values from 0 to 7, all different within a row; in each aligned block of 8 rows (0 to 7, 8 to 15, ...) at most 3 rows name the same one
- route_weights: float32 [1024, 2], replicated, may hold values from 0.2 to 1
Outputs:
- output: bfloat16 [1024, 2048], P('ep')
The draws below stay inside these ranges and needn't reach their ends.
Inputs may be any that keep to these rules, and one draw needn't show every extreme that they name: `routes`: each row names 2 different experts; the rows of one device (8 aligned rows) name one expert at most 3 times. `cum_gates`: non-increasing along positions.
All inputs are finite; a program needn't handle non-finite values.
Results may differ from the reference program's by a relative error of at most 0.012.
Values may be sent and summed in bfloat16 or wider, within the bound.
No kernel may reach another device: no remote copies, remote signals or barrier semaphores. Data moves between devices by JAX's collectives and lax.ppermute only.
A program may use at most 128 MiB of HBM per device.

```python
import math
import jax
import jax.numpy as jnp
import numpy as np
from jax import lax

D = 2048
HEADS = 32
HEAD_DIM = 64
KEY_VALUE_HEADS = 2
FF_DENSE = 5632
FF_EXPERT = 7168
EXPERTS = 8
TOP = 2
SEQ_DEV = 8
CACHE_SLOTS = 1024
SEQUENCE_COUNT = 1024
CAP = 3
N_EP = 128


def draw_cache_keys(key, part):
    key_rows = jax.random.split(key, 1)
    shape = (SEQUENCE_COUNT, CACHE_SLOTS, KEY_VALUE_HEADS * HEAD_DIM)
    return jax.random.normal(key_rows[0], shape, jnp.float32).astype(jnp.bfloat16)


def draw_cum_gates(key, part):
    key_rows = jax.random.split(key, 7)
    devices = SEQUENCE_COUNT // SEQ_DEV
    share_fast = 0.5
    fast = jax.random.uniform(key_rows[0], (SEQUENCE_COUNT, 1, KEY_VALUE_HEADS)) < share_fast
    fast_rate = jnp.exp(jax.random.uniform(key_rows[1], (SEQUENCE_COUNT, 1, KEY_VALUE_HEADS), jnp.float32, math.log(1.0 / 100.0), math.log(1.0 / 30.0)))
    slow_rate = jnp.exp(jax.random.uniform(key_rows[2], (SEQUENCE_COUNT, 1, KEY_VALUE_HEADS), jnp.float32, math.log(0.1), math.log(0.4))) / CACHE_SLOTS
    decay_rate = jnp.where(fast, fast_rate, slow_rate)
    per_device_ratio = jnp.exp(jax.random.uniform(key_rows[3], (devices, 1, 1), jnp.float32, 0.0, math.log(3.0)))
    per_device_ratio = jnp.repeat(per_device_ratio, SEQ_DEV, axis=0)
    coarse_estimate = jnp.exp(jax.random.uniform(key_rows[4], (SEQUENCE_COUNT, CACHE_SLOTS, KEY_VALUE_HEADS), jnp.float32, math.log(0.5), math.log(2.0)))
    spike_position = jax.random.randint(key_rows[5], (SEQUENCE_COUNT, 1, KEY_VALUE_HEADS, 2), 0, CACHE_SLOTS)
    decay_penalty = jax.random.uniform(key_rows[6], (SEQUENCE_COUNT, 1, KEY_VALUE_HEADS, 2), jnp.float32, 0.2, 0.5)
    current_slot = jnp.arange(CACHE_SLOTS, dtype=jnp.int32)[None, :, None, None]
    spike_amount = jnp.sum(jnp.where(current_slot == spike_position, -jnp.log(1.0 - decay_penalty), 0.0), axis=3)
    step_total = decay_rate * per_device_ratio * coarse_estimate + spike_amount
    return jnp.cumsum(-step_total, axis=1).astype(jnp.float32)


def with_ends(result, key, least, largest):
    longest = result.shape.index(max(result.shape))
    spots = []
    for shift in (0, 1):
        where = [jax.random.randint(jax.random.fold_in(key, axis), (), 0, length) for axis, length in enumerate(result.shape)]
        where[longest] = (where[longest] + shift) % result.shape[longest]
        spots.append(tuple(where))
    return result.at[spots[0]].set(least).at[spots[1]].set(largest)


def levels(stream_key, dims, cuts, smallest, top_value):
    level, own = 1.0, jax.random.fold_in(stream_key, 6)
    for dim, parts in cuts:
        heights = jnp.exp(jax.random.uniform(jax.random.fold_in(own, dim), (parts,), jnp.float32, smallest / len(cuts), top_value / len(cuts)))
        level = level * jnp.repeat(heights, dims[dim] // parts).reshape([-1 if axis == dim else 1 for axis in range(len(dims))])
    return level


def routed_block(stream_key, own, number, rows, count, top, reach, slope):
    ranking = jax.random.permutation(stream_key, count)
    crowded, common = load_shares(count, rows * top, reach, slope, True), load_shares(count, rows * top, reach, slope, False)
    places = jnp.arange(count)

    def named(tallies, turn):
        used = int((tallies > 0).sum())
        fixed = max(1, used // 4)
        shifted = fixed + (places - fixed + turn * (used - fixed)) % max(1, count - fixed)
        return jnp.zeros((count,), jnp.int32).at[ranking[jnp.where(places < fixed, places, shifted)]].set(jnp.asarray(tallies, jnp.int32))

    tallies = jnp.where(number % 4 == 0, named(crowded, number // 4), named(common, number - number // 4 - 1))
    mixed = jax.random.permutation(jax.random.fold_in(own, 3), count)
    source_of, taker = mixed[0:count // 2 * 2:2], mixed[1:count // 2 * 2:2]
    slack = jnp.minimum(tallies[source_of] - 1, reach - tallies[taker]) // 2
    slack = jnp.where((source_of == ranking[0]) | (taker == ranking[0]) | (tallies[taker] == 0), 0, jnp.maximum(slack, 0))
    shifted = jax.random.randint(jax.random.fold_in(own, 4), (count // 2,), 0, 1 << 20) % (slack + 1)
    tallies = tallies.at[source_of].add(-shifted).at[taker].add(shifted)
    items = jnp.searchsorted(jnp.cumsum(tallies), jnp.arange(rows * top), side="right").astype(jnp.int32)
    table = items.reshape(top, rows).T
    table = table[jax.random.permutation(jax.random.fold_in(own, 1), rows)]
    turn = jax.random.randint(jax.random.fold_in(own, 2), (rows, 1), 0, top)
    return jnp.take_along_axis(table, (jnp.arange(top)[None, :] + turn) % top, axis=1)


def load_shares(count, total, bound, skew, full):
    weights = [(1 << 20) // math.isqrt(rank ** skew) + 1 for rank in range(1, count + 1)]
    largest = bound if full else min(bound, max(-(-total // count), total * weights[0] // sum(weights)))
    least = 1 if total - largest >= count - 1 else 0
    holding, spare = [largest] + [least] * (count - 1), total - largest - least * (count - 1)
    while spare > 0:
        movable = [i for i in range(1, count) if holding[i] < largest] or [i for i in range(1, count) if holding[i] < bound]
        whole, remaining = sum([weights[i] for i in movable]), spare
        for i in movable:
            more = min(bound - holding[i], max(1, remaining * weights[i] // whole), spare)
            holding[i] = holding[i] + more
            spare = spare - more
    return np.array(holding)


def normal_values(stream_key, shape, scale, reach, cuts=(), held_as=jnp.bfloat16):
    level = levels(stream_key, shape, cuts, -0.22, 0.18) if cuts else 1.0
    values = jax.random.normal(stream_key, shape, jnp.float32) * scale * level
    return jnp.minimum(jnp.maximum(values, -reach), reach).astype(held_as)


def setup_inputs(seed: int = 0) -> dict:
    keys = jax.random.split(jax.random.key(seed), 22)
    tokens = normal_values(keys[0], (SEQUENCE_COUNT, D), 1.0, 6.0, ((0, 128),))
    cache_keys = draw_cache_keys(jax.random.fold_in(keys[21], 71), 0)
    cache_values = normal_values(keys[2], (SEQUENCE_COUNT, CACHE_SLOTS, KEY_VALUE_HEADS * HEAD_DIM), 1.0, 6.0, ((0, 128),))
    cum_gates = draw_cum_gates(jax.random.fold_in(keys[21], 71), 0)
    lengths = with_ends(jax.random.randint(keys[4], (SEQUENCE_COUNT,), CACHE_SLOTS // 8, CACHE_SLOTS + 1), jax.random.fold_in(keys[4], 1), CACHE_SLOTS // 8, CACHE_SLOTS).astype(jnp.int32)
    query_weight = normal_values(keys[5], (D, HEADS * HEAD_DIM), D ** -0.5, 0.125)
    key_weight = normal_values(keys[6], (D, KEY_VALUE_HEADS * HEAD_DIM), D ** -0.5, 0.125)
    value_weight = normal_values(keys[7], (D, KEY_VALUE_HEADS * HEAD_DIM), D ** -0.5, 0.125)
    forget_weight = normal_values(keys[8], (D, KEY_VALUE_HEADS), D ** -0.5, 0.125)
    out_weight = normal_values(keys[9], (HEADS * HEAD_DIM, D), (HEADS * HEAD_DIM // 64) ** -0.5, 1.0, ((0, 128),))
    norm_gain = jnp.clip(1.0 + 0.18 * jax.random.normal(keys[10], (2, D), jnp.float32), 0.1, 1.9)
    norm_bias = normal_values(keys[11], (2, D), 0.2, 1.0, (), jnp.float32)
    dense_gate_weight = normal_values(keys[12], (D, FF_DENSE), D ** -0.5, 0.125, ((1, 128),))
    dense_up_weight = normal_values(keys[13], (D, FF_DENSE), D ** -0.5, 0.125, ((1, 128),))
    dense_down_weight = normal_values(keys[14], (FF_DENSE, D), FF_DENSE ** -0.5, 0.078125, ((0, 128),))
    dense_scale = jnp.clip(jax.random.uniform(keys[15], (D,), jnp.float32, 0.2, 1.5), 0.2, 1.5)
    expert_gate_weight = normal_values(keys[16], (D, EXPERTS * FF_EXPERT), D ** -0.5, 0.125, ((1, 128),))
    expert_up_weight = normal_values(keys[17], (D, EXPERTS * FF_EXPERT), D ** -0.5, 0.125, ((1, 128),))
    expert_down_weight = normal_values(keys[18], (EXPERTS * FF_EXPERT, D), FF_EXPERT ** -0.5, 0.0625, ((0, 128),))
    routes_keys = jax.random.split(jax.random.fold_in(keys[19], 1), SEQUENCE_COUNT // SEQ_DEV)
    routes_turns = jax.random.permutation(jax.random.fold_in(keys[19], 3), SEQUENCE_COUNT // SEQ_DEV)
    routes = jax.vmap(lambda own, number: routed_block(jax.random.fold_in(keys[19], 2), own, number, SEQ_DEV, EXPERTS, TOP, CAP, 2))(routes_keys, routes_turns).reshape((SEQUENCE_COUNT, TOP))
    route_weights = jnp.clip(jax.random.uniform(keys[20], (SEQUENCE_COUNT, TOP), jnp.float32, 0.2, 1.0), 0.2, 1.0)
    return dict(tokens=tokens, cache_keys=cache_keys, cache_values=cache_values, cum_gates=cum_gates, lengths=lengths, query_weight=query_weight, key_weight=key_weight, value_weight=value_weight, forget_weight=forget_weight, out_weight=out_weight, norm_gain=norm_gain, norm_bias=norm_bias, dense_gate_weight=dense_gate_weight, dense_up_weight=dense_up_weight, dense_down_weight=dense_down_weight, dense_scale=dense_scale, expert_gate_weight=expert_gate_weight, expert_up_weight=expert_up_weight, expert_down_weight=expert_down_weight, routes=routes, route_weights=route_weights)


residual_scale = 1.4142135
norm_eps = 1e-05

def layer_norm(values, gain_row, shift_row):
    centre = lax.optimization_barrier(jnp.mean(values, axis=-1, keepdims=True))
    centred = values - centre
    spread = lax.optimization_barrier(jnp.mean(centred * centred, axis=-1, keepdims=True))
    return (centred * lax.rsqrt(spread + norm_eps) * gain_row + shift_row).astype(jnp.bfloat16)

def attend_block(inputs):
    queries, cached_keys, cached_values, gate_sums, length_row, fresh_key, fresh_value, fresh_gate = inputs
    amount = queries.shape[0]
    grouped = HEADS // KEY_VALUE_HEADS
    query_grid_four = queries.astype(jnp.float32).reshape(amount, KEY_VALUE_HEADS, grouped, HEAD_DIM)
    key_four = cached_keys.astype(jnp.float32).reshape(amount, CACHE_SLOTS, KEY_VALUE_HEADS, HEAD_DIM)
    value_four = cached_values.astype(jnp.float32).reshape(amount, CACHE_SLOTS, KEY_VALUE_HEADS, HEAD_DIM)
    self_key_row = fresh_key.astype(jnp.float32).reshape(amount, KEY_VALUE_HEADS, HEAD_DIM)
    own_value = fresh_value.astype(jnp.float32).reshape(amount, KEY_VALUE_HEADS, HEAD_DIM)
    ratio_value = HEAD_DIM ** (-0.5)
    latest = jnp.take_along_axis(gate_sums, (length_row - 1).astype(jnp.int32)[:, None, None], axis=1)
    offsets = jnp.transpose(latest - gate_sums + fresh_gate[:, None, :], (0, 2, 1))
    past = jnp.einsum('bkgd,blkd->bkgl', query_grid_four, key_four) * ratio_value + offsets[:, :, None, :]
    live = jnp.arange(CACHE_SLOTS, dtype=jnp.int32)[None, :] < length_row[:, None]
    past = jnp.where(live[:, None, None, :], past, -jnp.inf)
    self_part = jnp.einsum('rifs,ris->rif', query_grid_four, self_key_row) * ratio_value
    highest = jnp.maximum(lax.optimization_barrier(jnp.max(past, axis=-1)), self_part)
    past_exp = jnp.exp(past - highest[..., None])
    own_exp = jnp.exp(self_part - highest)
    denominator = lax.optimization_barrier(jnp.sum(past_exp, axis=-1)) + own_exp
    past_weight = lax.optimization_barrier((past_exp / denominator[..., None]).astype(jnp.bfloat16)).astype(jnp.float32)
    own_weight = lax.optimization_barrier((own_exp / denominator).astype(jnp.bfloat16)).astype(jnp.float32)
    mixed = jnp.einsum('bkgl,blkd->bkgd', past_weight, value_four) + own_weight[..., None] * own_value[:, :, None, :]
    return mixed.reshape(amount, HEADS * HEAD_DIM).astype(jnp.bfloat16)

def expert_mix(settled, expert_gate, expert_up, expert_down, routes, route_weights):
    shards = N_EP // EXPERTS
    part_width = FF_EXPERT // shards
    chosen = routes.reshape(N_EP, SEQ_DEV, TOP)
    shares = route_weights.reshape(N_EP, SEQ_DEV, TOP)
    expert_ids = jnp.arange(EXPERTS, dtype=jnp.int32)
    picked = (chosen[..., None] == expert_ids).astype(jnp.int32)
    hits = lax.optimization_barrier(jnp.sum(picked, axis=2))
    portion = lax.optimization_barrier(jnp.sum(picked.astype(jnp.float32) * shares[..., None], axis=2))
    ranks = jnp.cumsum(hits, axis=1) - hits
    slot_ids = jnp.arange(CAP, dtype=jnp.int32)
    matched = (hits[..., None] * (ranks[..., None] == slot_ids).astype(jnp.int32)).astype(jnp.float32)
    by_source = settled.astype(jnp.float32).reshape(N_EP, SEQ_DEV, D)

    def one_expert(running, expert):
        select = lax.dynamic_index_in_dim(matched, expert, 2, keepdims=False)
        weight_here = lax.dynamic_index_in_dim(portion, expert, 2, keepdims=False)
        slot_rows = jnp.einsum('nsc,nsd->ncd', select, by_source, precision=lax.Precision.HIGHEST)
        slot_rows = slot_rows.reshape(N_EP * CAP, D).astype(jnp.bfloat16)
        gate_cols = lax.dynamic_slice_in_dim(expert_gate, expert * FF_EXPERT, FF_EXPERT, 1)
        up_cols = lax.dynamic_slice_in_dim(expert_up, expert * FF_EXPERT, FF_EXPERT, 1)
        down_rows = lax.dynamic_slice_in_dim(expert_down, expert * FF_EXPERT, FF_EXPERT, 0)
        gate_val = jnp.dot(slot_rows, gate_cols, preferred_element_type=jnp.float32)
        up_val = jnp.dot(slot_rows, up_cols, preferred_element_type=jnp.float32)
        hidden = (jax.nn.silu(gate_val) * up_val).astype(jnp.bfloat16)
        pieces = jnp.einsum('rgf,gfd->rgd', hidden.astype(jnp.float32).reshape(N_EP * CAP, shards, part_width), down_rows.astype(jnp.float32).reshape(shards, part_width, D))
        pieces = lax.optimization_barrier(pieces.astype(jnp.bfloat16)).astype(jnp.float32)
        summed = lax.optimization_barrier(jnp.sum(pieces, axis=1)).reshape(N_EP, CAP, D)
        placed = jnp.einsum('nsc,ncd->nsd', select, summed, precision=lax.Precision.HIGHEST)
        return (running + weight_here[..., None] * placed, None)
    combined, unused = lax.scan(one_expert, jnp.zeros((N_EP, SEQ_DEV, D), jnp.float32), jnp.arange(EXPERTS, dtype=jnp.int32))
    return combined.reshape(N_EP * SEQ_DEV, D)

def reference(tokens, cache_keys, cache_values, cum_gates, lengths, query_weight, key_weight, value_weight, forget_weight, out_weight, norm_gain, norm_bias, dense_gate_weight, dense_up_weight, dense_down_weight, dense_scale, expert_gate_weight, expert_up_weight, expert_down_weight, routes, route_weights):
    query = jnp.dot(tokens, query_weight, preferred_element_type=jnp.float32).astype(jnp.bfloat16)
    new_key = jnp.dot(tokens, key_weight, preferred_element_type=jnp.float32).astype(jnp.bfloat16)
    new_value = jnp.dot(tokens, value_weight, preferred_element_type=jnp.float32).astype(jnp.bfloat16)
    new_gate = jax.nn.log_sigmoid(jnp.dot(tokens, forget_weight, preferred_element_type=jnp.float32))

    def blocks(array):
        return array.reshape((N_EP, SEQ_DEV) + array.shape[1:])
    attended = lax.map(attend_block, (blocks(query), blocks(cache_keys), blocks(cache_values), blocks(cum_gates), blocks(lengths), blocks(new_key), blocks(new_value), blocks(new_gate)))
    attended = attended.reshape(SEQUENCE_COUNT, HEADS * HEAD_DIM)
    projected = jnp.dot(attended, out_weight, preferred_element_type=jnp.float32)
    settled = layer_norm(residual_scale * tokens.astype(jnp.float32) + projected, norm_gain[0], norm_bias[0])
    dense_gate = jnp.dot(settled, dense_gate_weight, preferred_element_type=jnp.float32)
    dense_up = jnp.dot(settled, dense_up_weight, preferred_element_type=jnp.float32)
    dense_hidden = (jax.nn.silu(dense_gate) * dense_up).astype(jnp.bfloat16)
    dense_out = jnp.dot(dense_hidden, dense_down_weight, preferred_element_type=jnp.float32)
    expert_out = expert_mix(settled, expert_gate_weight, expert_up_weight, expert_down_weight, routes, route_weights)
    ffn = expert_out + dense_scale * dense_out
    return layer_norm(residual_scale * settled.astype(jnp.float32) + ffn, norm_gain[1], norm_bias[1])
```

```python
import jax
import jax.numpy as jnp
from jax import lax
from jax.sharding import PartitionSpec as P

EXPERTS = 8
TOP = 2
CAP = 3


residual_scale = 1.4142135
norm_eps = 1e-05


CHIPS = 64
SLOTS = 5
GROUP_Z = 4

CORE_GROUPS = [[2 * chip + core for chip in range(64)] for core in range(2)]
ROW_GROUPS = [[8 * ring + place for place in range(8)] for ring in range(16)]
WEIGHT_GROUPS = [[8 * ring + place for ring in range(16)] for place in range(8)]


def shift_z(block, step):
    return lax.ppermute(block, "ep", [(i, (i + 32 * step) % 128) for i in range(128)])


def swap_core(block):
    return lax.ppermute(block, "ep", [(i, i ^ 1) for i in range(128)])


def exchange(block, groups):
    return lax.all_to_all(
        block, "ep", split_axis=0, concat_axis=0, axis_index_groups=groups, tiled=True
    )


def layer_norm(values, gain_row, shift_row):
    centre = jnp.mean(values, axis=-1, keepdims=True)
    centred = values - centre
    spread = jnp.mean(centred * centred, axis=-1, keepdims=True)
    return (centred * lax.rsqrt(spread + norm_eps) * gain_row + shift_row).astype(jnp.bfloat16)


def attend(
    queries, cached_keys, cached_values, gate_sums, length_row, fresh_key, fresh_value, fresh_gate
):
    amount = queries.shape[0]
    cache_len = cached_keys.shape[1]
    kv_count = fresh_gate.shape[1]
    head_dim = fresh_key.shape[1] // kv_count
    grouped = queries.shape[1] // (kv_count * head_dim)
    query_grid_four = queries.reshape(amount, kv_count, grouped, head_dim)
    key_four = cached_keys.reshape(amount, cache_len, kv_count, head_dim)
    value_four = cached_values.reshape(amount, cache_len, kv_count, head_dim)
    self_key_row = fresh_key.reshape(amount, kv_count, head_dim)
    own_value = fresh_value.astype(jnp.float32).reshape(amount, kv_count, head_dim)
    ratio_value = head_dim ** (-0.5)
    latest = jnp.take_along_axis(gate_sums, (length_row - 1)[:, None, None], axis=1)
    offsets = jnp.transpose(latest - gate_sums + fresh_gate[:, None, :], (0, 2, 1))
    past = jnp.einsum(
        "bkgd,blkd->bkgl", query_grid_four, key_four, preferred_element_type=jnp.float32
    )
    past = past * ratio_value + offsets[:, :, None, :]
    live = jnp.arange(cache_len, dtype=jnp.int32)[None, :] < length_row[:, None]
    past = jnp.where(live[:, None, None, :], past, -jnp.inf)
    self_part = (
        jnp.einsum(
            "rifs,ris->rif", query_grid_four, self_key_row, preferred_element_type=jnp.float32
        )
        * ratio_value
    )
    highest = jnp.maximum(jnp.max(past, axis=-1), self_part)
    past_exp = jnp.exp(past - highest[..., None])
    own_exp = jnp.exp(self_part - highest)
    denominator = jnp.sum(past_exp, axis=-1) + own_exp
    past_weight = (past_exp / denominator[..., None]).astype(jnp.bfloat16)
    own_weight = (own_exp / denominator).astype(jnp.bfloat16)
    mixed = jnp.einsum(
        "bkgl,blkd->bkgd", past_weight, value_four, preferred_element_type=jnp.float32
    )
    mixed = mixed + own_weight.astype(jnp.float32)[..., None] * own_value[:, :, None, :]
    return mixed.reshape(amount, queries.shape[1]).astype(jnp.bfloat16)


def slot_tables(chosen, shares):
    expert_ids = jnp.arange(EXPERTS, dtype=jnp.int32)
    picked = (chosen[..., None] == expert_ids).astype(jnp.int32)
    hits = jnp.sum(picked, axis=1)
    portion = jnp.sum(picked.astype(jnp.float32) * shares[..., None], axis=1)
    ranks = jnp.cumsum(hits, axis=0) - hits
    slot_ids = jnp.arange(CAP, dtype=jnp.int32)
    matched = (hits[..., None] * (ranks[..., None] == slot_ids).astype(jnp.int32)).astype(
        jnp.float32
    )
    return (matched, portion)


def gather_dense(gate_cols, up_cols, down_rows):
    short = ((0, 4), (0, 0))
    own = jnp.concatenate(
        [
            jnp.pad(jnp.transpose(gate_cols), short),
            jnp.pad(jnp.transpose(up_cols), short),
            jnp.pad(down_rows, short),
        ],
        axis=0,
    )
    half = own.shape[0] // 2
    before = shift_z(own, 1)
    after = shift_z(own, -1)
    far_low = shift_z(before[:half], 1)
    far_high = shift_z(after[half:], -1)
    mine = jnp.concatenate([own, before, after, far_low, far_high], axis=0)
    both = jnp.concatenate([mine, swap_core(mine)], axis=0)
    parts = both.reshape(8, 3, 48, 2048)
    return [parts[:, i].reshape(384, 2048) for i in range(3)]


def local(
    tokens,
    cache_keys,
    cache_values,
    cum_gates,
    lengths,
    query_weight,
    key_weight,
    value_weight,
    forget_weight,
    out_weight,
    norm_gain,
    norm_bias,
    dense_gate_weight,
    dense_up_weight,
    dense_down_weight,
    dense_scale,
    expert_gate_weight,
    expert_up_weight,
    expert_down_weight,
    routes,
    route_weights,
):
    own_index = lax.axis_index("ep")
    rows, width = tokens.shape
    out_rows = exchange(jnp.tile(out_weight, (16, 1)), WEIGHT_GROUPS)
    dense_gate_rows, dense_up_rows, dense_down_all = gather_dense(
        dense_gate_weight, dense_up_weight, dense_down_weight
    )
    query = jnp.dot(tokens, query_weight, preferred_element_type=jnp.float32).astype(jnp.bfloat16)
    new_key = jnp.dot(tokens, key_weight, preferred_element_type=jnp.float32).astype(jnp.bfloat16)
    new_value = jnp.dot(tokens, value_weight, preferred_element_type=jnp.float32).astype(
        jnp.bfloat16
    )
    new_gate = jax.nn.log_sigmoid(
        jnp.dot(tokens, forget_weight, preferred_element_type=jnp.float32)
    )
    attended = attend(
        query, cache_keys, cache_values, cum_gates, lengths, new_key, new_value, new_gate
    )
    slices = jnp.transpose(attended.reshape(rows, 16, 8, 16), (2, 0, 1, 3)).reshape(64, 256)
    slices = exchange(slices, ROW_GROUPS)
    partial = jnp.dot(slices, out_rows, preferred_element_type=jnp.float32).astype(jnp.bfloat16)
    partial = exchange(partial, ROW_GROUPS)
    projected = jnp.sum(partial.reshape(8, rows, width).astype(jnp.float32), axis=0)
    settled = layer_norm(
        residual_scale * tokens.astype(jnp.float32) + projected, norm_gain[0], norm_bias[0]
    )
    own_routes = lax.dynamic_slice_in_dim(routes, own_index * rows, rows, 0)
    own_shares = lax.dynamic_slice_in_dim(route_weights, own_index * rows, rows, 0)
    matched, portion = slot_tables(own_routes, own_shares)
    expert_ids = jnp.arange(EXPERTS, dtype=jnp.int32)
    pair_row = 2 * (expert_ids // 2)[:, None] + jnp.arange(2, dtype=jnp.int32)[None, :]
    dense_pick = (pair_row[..., None] == jnp.arange(rows, dtype=jnp.int32)).astype(jnp.bfloat16)
    picks = jnp.concatenate(
        [jnp.transpose(matched, (1, 2, 0)).astype(jnp.bfloat16), dense_pick], axis=1
    )
    messages = jnp.einsum(
        "ekr,rsc->eskc",
        picks,
        settled.reshape(rows, 8, 256),
        preferred_element_type=jnp.float32,
    ).astype(jnp.bfloat16)
    outgoing = jnp.repeat(messages.reshape(EXPERTS, 1, 8, SLOTS * 256), 8, axis=1)
    received = exchange(outgoing.reshape(CHIPS * 8, SLOTS * 256), CORE_GROUPS)
    arrived = jnp.transpose(received.reshape(CHIPS, 8, SLOTS, 256), (2, 0, 1, 3)).reshape(
        SLOTS, CHIPS, width
    )
    expert_rows = arrived[:CAP].reshape(CAP * CHIPS, width)
    dense_rows = arrived[CAP:].reshape(2 * CHIPS, width)
    other_rows = swap_core(expert_rows)
    contract = (((1,), (1,)), ((), ()))
    gate_val = lax.dot_general(
        dense_rows, dense_gate_rows, contract, preferred_element_type=jnp.float32
    )
    up_val = lax.dot_general(
        dense_rows, dense_up_rows, contract, preferred_element_type=jnp.float32
    )
    dense_hidden = (jax.nn.silu(gate_val) * up_val).astype(jnp.bfloat16)
    dense_part = jnp.dot(dense_hidden, dense_down_all, preferred_element_type=jnp.float32)
    both_rows = jnp.concatenate([expert_rows, other_rows], axis=0)
    gate_val = jnp.dot(both_rows, expert_gate_weight, preferred_element_type=jnp.float32)
    up_val = jnp.dot(both_rows, expert_up_weight, preferred_element_type=jnp.float32)
    hidden = (jax.nn.silu(gate_val) * up_val).astype(jnp.bfloat16)
    result = jnp.dot(hidden, expert_down_weight, preferred_element_type=jnp.float32)
    half = CAP * CHIPS
    result_mine = result[:half] + swap_core(result[half:].astype(jnp.bfloat16)).astype(jnp.float32)
    answers = jnp.concatenate([result_mine, dense_part], axis=0).astype(jnp.bfloat16)
    answers = jnp.transpose(answers.reshape(SLOTS, CHIPS, 8, 256), (1, 2, 0, 3))
    returned = exchange(answers.reshape(CHIPS * 8, SLOTS * 256), CORE_GROUPS)
    returned = returned.reshape(CHIPS, 8, SLOTS, 256).astype(jnp.float32)
    expert_sum = jnp.sum(returned[:, :, :CAP].reshape(EXPERTS, 8, 8, CAP, 256), axis=1)
    dense_sum = jnp.sum(returned[:, :, CAP:].reshape(GROUP_Z, 16, 8, 2, 256), axis=1)
    dense_out = jnp.transpose(dense_sum, (0, 2, 1, 3)).reshape(rows, width)
    expert_out = jnp.einsum("rek,eskc->rsc", matched * portion[..., None], expert_sum).reshape(
        rows, width
    )
    ffn = dense_scale * dense_out + expert_out
    return layer_norm(
        residual_scale * settled.astype(jnp.float32) + ffn, norm_gain[1], norm_bias[1]
    )


def solution(mesh):
    return jax.shard_map(
        local,
        mesh=mesh,
        in_specs=(
            P("ep", None),
            P("ep", None, None),
            P("ep", None, None),
            P("ep", None, None),
            P("ep"),
            P(),
            P(),
            P(),
            P(),
            P("ep", None),
            P(),
            P(),
            P(None, "ep"),
            P(None, "ep"),
            P("ep", None),
            P(),
            P(None, "ep"),
            P(None, "ep"),
            P("ep", None),
            P(),
            P(),
        ),
        out_specs=P("ep", None),
        check_vma=False,
    )
```
